32 devices in a mesh: sp: 8 (over z, y), tp: 4 (over x, core).
Axes of the slice: x: 2, y: 2, z: 4, core: 2. Of those that a mesh axis runs over, the one named last changes fastest.
Arguments:
- query_first: bfloat16 [6144, 8, 128], P('sp', 'tp'), may hold values from -5.375 to 5.375
- key_first: bfloat16 [6144, 8, 128], P('sp', 'tp'), may hold values from -5.375 to 5.375
- value_first: bfloat16 [6144, 8, 128], P('sp', 'tp'), may hold values from -6 to 6
- query_second: bfloat16 [6144, 8, 256], P('sp', 'tp'), may hold values from -5.375 to 5.375
- key_second: bfloat16 [6144, 8, 256], P('sp', 'tp'), may hold values from -5.375 to 5.375
- value_second: bfloat16 [6144, 8, 128], P('sp', 'tp'), may hold values from -6 to 6
- mix_lambda: float32 [2, 8], P(None, 'tp'), may hold values from 0.3 to 0.8
- head_gain: float32 [2, 8, 128], P(None, 'tp'), may hold values from 0.1 to 1.9
- out_weight: bfloat16 [2, 8, 128, 2048], P(None, 'tp'), may hold values from -0.125 to 0.125
- residual: bfloat16 [6144, 2048], P(('sp', 'tp')), may hold values from -6 to 6
- norm_gain: float32 [2, 2048], replicated, may hold values from 0.1 to 1.9
- up_weight: bfloat16 [2048, 8192], P('sp', 'tp'), may hold values from -0.125 to 0.125
- down_weight: bfloat16 [8192, 2048], P('tp', 'sp'), may hold values from -0.0625 to 0.0625
Outputs:
- mixed: bfloat16 [6144, 2048], P(('sp', 'tp'))
The draws below stay inside these ranges and needn't reach their ends.
All inputs are finite; a program needn't handle non-finite values.
Results may differ from the reference program's by a relative error of at most 0.02.
Values may be sent and summed in bfloat16 or wider, within the bound.
No kernel may reach another device: no remote copies, remote signals or barrier semaphores. Data moves between devices by JAX's collectives and lax.ppermute only.
A program may use at most 128 MiB of HBM per device.

```python
import math
import jax
import jax.numpy as jnp
from jax import lax

D = 2048
FF = 8192
HEADS = 8
KA = 64
KB = 128
VD = 128
TOK_DEV = 768
TOKENS = 6144
N_SP = 8


def drawn_pair(key, group_tag, key_size):
    seeded = jax.random.fold_in(key, group_tag)
    seed_query, seed_keys = jax.random.split(seeded, 2)
    array_shape = (TOKENS, HEADS, 2 * key_size)
    queries = 1.3 * jax.random.truncated_normal(seed_query, -3.4, 3.4, array_shape, jnp.float32)
    key_rows = 1.3 * jax.random.truncated_normal(seed_keys, -3.4, 3.4, array_shape, jnp.float32)
    return (queries, key_rows)


def draw_query_first(key, part):
    return drawn_pair(key, 11, KA)[0].astype(jnp.bfloat16)


def draw_key_first(key, part):
    return drawn_pair(key, 11, KA)[1].astype(jnp.bfloat16)


def draw_query_second(key, part):
    return drawn_pair(key, 23, KB)[0].astype(jnp.bfloat16)


def draw_key_second(key, part):
    return drawn_pair(key, 23, KB)[1].astype(jnp.bfloat16)


def shard_levels(own_key, dims, cuts, smallest, high):
    def one(position, blocks):
        heights = jax.random.uniform(jax.random.fold_in(jax.random.fold_in(own_key, 6), position), (blocks,), jnp.float32, smallest / len(cuts), high / len(cuts))
        return jnp.repeat(jnp.exp(heights), dims[position] // blocks).reshape((-1,) + (1,) * (len(dims) - position - 1))

    loudness = one(*cuts[0])
    for cut in cuts[1:]:
        loudness = loudness * one(*cut)
    return loudness


def scatter_about(key, shape, deviation, limit, cuts=(), kind=jnp.bfloat16):
    drawn = deviation * jax.random.normal(key, shape, jnp.float32)
    if cuts:
        drawn = drawn * shard_levels(key, shape, cuts, -0.22, 0.18)
    return jnp.clip(drawn, -limit, limit).astype(kind)


def setup_inputs(seed: int = 0) -> dict:
    seeds = jax.random.split(jax.random.key(seed), 14)
    return {
        "query_first": draw_query_first(jax.random.fold_in(seeds[13], 71), 0),
        "key_first": draw_key_first(jax.random.fold_in(seeds[13], 71), 0),
        "value_first": scatter_about(seeds[2], (TOKENS, HEADS, VD), 1.0, 6.0, ((0, 8), (1, 4))),
        "query_second": draw_query_second(jax.random.fold_in(seeds[13], 71), 0),
        "key_second": draw_key_second(jax.random.fold_in(seeds[13], 71), 0),
        "value_second": scatter_about(seeds[5], (TOKENS, HEADS, VD), 1.0, 6.0, ((0, 8), (1, 4))),
        "mix_lambda": jnp.clip(0.3 + 0.5 * jax.random.uniform(seeds[6], (2, HEADS), jnp.float32) ** shard_levels(seeds[6], (2, HEADS), ((1, 4),), -0.2, 0.2), 0.3, 0.8),
        "head_gain": jnp.clip(1.0 + 0.18 * jax.random.normal(seeds[7], (2, HEADS, VD), jnp.float32), 0.1, 1.9),
        "out_weight": scatter_about(seeds[8], (2, HEADS, VD, D), D ** -0.5, 0.125, ((1, 4),)),
        "residual": scatter_about(seeds[9], (TOKENS, D), 1.0, 6.0, ((0, 32),)),
        "norm_gain": jnp.clip(1.0 + 0.18 * jax.random.normal(seeds[10], (2, D), jnp.float32), 0.1, 1.9),
        "up_weight": scatter_about(seeds[11], (D, FF), D ** -0.5, 0.125, ((0, 8), (1, 4))),
        "down_weight": scatter_about(seeds[12], (FF, D), FF ** -0.5, 0.0625, ((0, 4), (1, 8))),
    }


EPSILON = 1e-05

def layer_norm(activations, scales):
    average = lax.optimization_barrier(jnp.mean(activations, axis=-1, keepdims=True))
    centred = activations - average
    spread = lax.optimization_barrier(jnp.mean(centred * centred, axis=-1, keepdims=True))
    return centred * lax.rsqrt(spread + EPSILON) * scales

def group_attention(queries_in, keys_in, values_in, lambdas, gains, key_size):
    score_scale = 1.0 / math.sqrt(key_size)
    queries = queries_in.astype(jnp.float32).reshape(TOKENS, HEADS, 2, key_size)
    key_rows = keys_in.astype(jnp.float32).reshape(TOKENS, HEADS, 2, key_size)
    value_rows = values_in.astype(jnp.float32)
    query_blocks = queries.reshape(N_SP, TOK_DEV, HEADS, 2, key_size)

    def one_block(query_block):
        scores = jnp.einsum('qhck,phck->hcqp', query_block, key_rows) * score_scale
        peak = lax.optimization_barrier(jnp.max(scores, axis=-1, keepdims=True))
        exponent = jnp.exp(scores - peak)
        denominator = lax.optimization_barrier(jnp.sum(exponent, axis=-1))
        rounded = lax.optimization_barrier(exponent.astype(jnp.bfloat16)).astype(jnp.float32)
        numerator = jnp.einsum('hcqp,phv->hcqv', rounded, value_rows)
        attended = numerator[:, 0] / denominator[:, 0, :, None] - lambdas[:, None, None] * numerator[:, 1] / denominator[:, 1, :, None]
        mean_square = lax.optimization_barrier(jnp.mean(attended * attended, axis=-1, keepdims=True))
        return (attended * lax.rsqrt(mean_square + EPSILON) * gains[:, None, :]).astype(jnp.bfloat16)
    blocks_out = lax.map(one_block, query_blocks)
    return blocks_out.transpose(1, 0, 2, 3).reshape(HEADS, TOKENS, VD)

def reference(query_first, key_first, value_first, query_second, key_second, value_second, mix_lambda, head_gain, out_weight, residual, norm_gain, up_weight, down_weight):
    heads_first = group_attention(query_first, key_first, value_first, mix_lambda[0], head_gain[0], KA)
    heads_second = group_attention(query_second, key_second, value_second, mix_lambda[1], head_gain[1], KB)
    stacked = jnp.stack([heads_first, heads_second]).astype(jnp.float32)
    projected = jnp.einsum('ghtv,ghvd->td', stacked, out_weight.astype(jnp.float32)) + residual.astype(jnp.float32)
    normed = layer_norm(projected, norm_gain[0])
    expanded = jnp.dot(normed.astype(jnp.bfloat16), up_weight, preferred_element_type=jnp.float32)
    hidden = jnp.square(jnp.maximum(expanded, 0.0)).astype(jnp.bfloat16)
    mixed_sum = jnp.dot(hidden, down_weight, preferred_element_type=jnp.float32)
    return layer_norm(normed + mixed_sum, norm_gain[1]).astype(jnp.bfloat16)
```

```python
import functools
import math

import jax
import jax.numpy as jnp
from jax import lax
from jax.experimental import pallas as pl
from jax.experimental.pallas import tpu as pltpu
from jax.sharding import PartitionSpec as P

EPSILON = 1e-05
LOG2_E = math.log2(math.e)
AXES = ("sp", "tp")


def layer_norm(activations, scales):
    average = jnp.mean(activations, axis=-1, keepdims=True)
    centred = activations - average
    spread = jnp.mean(centred * centred, axis=-1, keepdims=True)
    return centred * lax.rsqrt(spread + EPSILON) * scales


def attend_body(scal_ref, mask_ref, gain_ref, q_ref, k_ref, v_ref, out_ref, *, key_block):
    rows = q_ref.shape[0]
    keys = k_ref.shape[0]
    queries = q_ref[...]
    both = jnp.concatenate([queries * mask_ref[0:1, :], queries * mask_ref[1:2, :]], axis=0)
    scale = scal_ref[0]
    top = total = numerator = None
    for start in range(0, keys, key_block):
        scores = lax.dot_general(
            both,
            k_ref[start : start + key_block, :],
            (((1,), (1,)), ((), ())),
            preferred_element_type=jnp.float32,
        )
        scores = scores * scale
        block_top = jnp.max(scores, axis=-1, keepdims=True)
        newest = block_top if top is None else jnp.maximum(top, block_top)
        weights = jnp.exp2(scores - newest)
        block_total = jnp.sum(weights, axis=-1, keepdims=True)
        block_numerator = jnp.dot(
            weights.astype(jnp.bfloat16),
            v_ref[start : start + key_block, :],
            preferred_element_type=jnp.float32,
        )
        if top is None:
            total, numerator = block_total, block_numerator
        else:
            factor = jnp.exp2(top - newest)
            total = total * factor + block_total
            numerator = numerator * factor + block_numerator
        top = newest
    ratio = numerator / total
    attended = ratio[:rows] - scal_ref[1] * ratio[rows:]
    mean_square = jnp.mean(attended * attended, axis=-1, keepdims=True)
    out_ref[...] = (attended * lax.rsqrt(mean_square + EPSILON) * gain_ref[...]).astype(out_ref.dtype)


def attend(scalars, masks, gain, queries, keys, values, query_block, key_block):
    count, width = queries.shape
    length, value_size = values.shape
    return pl.pallas_call(
        functools.partial(attend_body, key_block=key_block),
        grid=(count // query_block,),
        in_specs=[
            pl.BlockSpec(memory_space=pltpu.SMEM),
            pl.BlockSpec((2, width), lambda i: (0, 0)),
            pl.BlockSpec((1, value_size), lambda i: (0, 0)),
            pl.BlockSpec((query_block, width), lambda i: (i, 0)),
            pl.BlockSpec((length, width), lambda i: (0, 0)),
            pl.BlockSpec((length, value_size), lambda i: (0, 0)),
        ],
        out_specs=pl.BlockSpec((query_block, value_size), lambda i: (i, 0)),
        out_shape=jax.ShapeDtypeStruct((count, value_size), jnp.bfloat16),
        compiler_params=pltpu.CompilerParams(vmem_limit_bytes=56 * 1024 * 1024),
        cost_estimate=pl.CostEstimate(
            flops=4 * count * length * (width + value_size),
            bytes_accessed=2 * (count + length) * (width + value_size),
            transcendentals=2 * count * length,
        ),
        name="attend",
    )(scalars, masks, gain, queries, keys, values)


def solution(mesh):
    n_sp, n_tp = mesh.shape["sp"], mesh.shape["tp"]

    def pairs(move):
        listed = []
        for s in range(n_sp):
            for t in range(n_tp):
                target = move(s, t)
                if target is not None:
                    listed.append((s * n_tp + t, target[0] * n_tp + target[1]))
        return listed

    def send(array, move):
        return lax.ppermute(array, AXES, pairs(move))

    def local(
        query_first,
        key_first,
        value_first,
        query_second,
        key_second,
        value_second,
        mix_lambda,
        head_gain,
        out_weight,
        residual,
        norm_gain,
        up_weight,
        down_weight,
    ):
        tok, heads, wide = query_first.shape
        size_first, size_second = wide // 2, query_second.shape[2] // 2
        value_size = value_first.shape[2]
        ways = 2 * heads
        stride = n_sp // ways
        sp, tp = lax.axis_index("sp"), lax.axis_index("tp")
        mine, lane = sp // stride, sp % stride
        is_second = mine >= heads

        def swap(s, t):
            return (s - s % 2 + t % 2, t - t % 2 + s % 2)

        def core(s, t):
            return (s, t ^ 1)

        lines = [[2 * z + y for z in range(n_sp // 2)] for y in range(2)]

        def by_head(array):
            return jnp.transpose(array, (1, 0, 2))

        def split_second(array):
            moved = by_head(array)
            return moved[:, :, :wide], moved[:, :, wide:]

        query_low, query_high = split_second(query_second)
        key_low, key_high = split_second(key_second)
        query_main = jnp.concatenate([by_head(query_first), query_low])
        key_main = jnp.concatenate([by_head(key_first), key_low])
        value_main = jnp.concatenate([by_head(value_first), by_head(value_second)])

        def pick(array, way):
            return lax.dynamic_index_in_dim(array, way, 0, keepdims=False)

        def shifted(step):
            return lambda s, t: ((s + step * stride) % n_sp, t)

        def shifted_high(step):
            def move(s, t):
                target = (s + step * stride) % n_sp
                return (target, t) if target // stride >= heads else None

            return move

        query_parts, key_parts, value_parts = [], [], []
        for step in range(ways):
            way = (mine + step) % ways
            upper = jnp.maximum(way - heads, 0)
            parts = (pick(query_main, way), pick(key_main, way), pick(value_main, way))
            highs = (pick(query_high, upper), pick(key_high, upper))
            if step == 0:
                highs = tuple(jnp.where(is_second, h, jnp.zeros_like(h)) for h in highs)
            else:
                parts = tuple(send(p, shifted(step)) for p in parts)
                highs = tuple(send(h, shifted_high(step)) for h in highs)
            query_parts.append(jnp.concatenate([parts[0], highs[0]], axis=1))
            key_parts.append([parts[1], highs[1]])
            value_parts.append(parts[2])

        def across(step):
            return lambda s, t: (s - s % stride + (s % stride + step) % stride, t)

        def across_high(step):
            def move(s, t):
                return across(step)(s, t) if s // stride >= heads else None

            return move

        key_rows, value_rows = [], []
        for step in range(ways):
            low, high = key_parts[step]
            key_rows.append(jnp.concatenate([low, high], axis=1))
            value_rows.append(value_parts[step])
            for other in range(1, stride):
                moved_low = send(low, across(other))
                moved_high = send(high, across_high(other))
                key_rows.append(jnp.concatenate([moved_low, moved_high], axis=1))
                value_rows.append(send(value_parts[step], across(other)))
        queries = jnp.concatenate(query_parts)
        keys = jnp.concatenate(key_rows)
        values = jnp.concatenate(value_rows)

        up_swapped, down_swapped = send(up_weight, swap), send(down_weight, swap)
        up_swapped, down_swapped, keys = lax.optimization_barrier((up_swapped, down_swapped, keys))
        up_own = lax.all_gather(up_swapped, "sp", axis_index_groups=lines, axis=0, tiled=True)
        down_own = lax.all_gather(down_swapped, "sp", axis_index_groups=lines, axis=0)
        up_other, down_other = send(up_own, core), send(down_own, core)

        lanes = jnp.arange(2 * wide)[None, :]
        half = jnp.where(is_second, wide, size_first)
        masks = jnp.concatenate([lanes < half, lanes >= half]).astype(jnp.bfloat16)
        scale = jnp.where(is_second, 1.0 / math.sqrt(size_second), 1.0 / math.sqrt(size_first))
        way_lambda = pick(mix_lambda.reshape(ways), mine)
        way_gain = pick(head_gain.reshape(ways, value_size), mine)
        scalars = jnp.stack([scale * LOG2_E, way_lambda]).astype(jnp.float32)
        head_out = attend(scalars, masks, way_gain[None, :], queries, keys, values, 256, 1024)

        returned = []
        for step in range(ways):
            part = head_out[step * tok : (step + 1) * tok]
            returned.append(part if step == 0 else send(part, shifted(-step)))
        returned = jnp.stack(returned)
        ordered = jnp.concatenate([pick(returned, (w - mine) % ways) for w in range(ways)], axis=1)
        rows = tok // n_tp
        weight_rows = out_weight.reshape(ways * value_size, out_weight.shape[-1])
        projected = residual.astype(jnp.float32)
        for bit in range(n_tp):
            part = lax.dynamic_slice_in_dim(ordered, (tp ^ bit) * rows, rows, 0)
            weight = weight_rows
            if bit:
                flip = lambda s, t, bit=bit: (s, t ^ bit)
                part, weight = send(part, flip), send(weight_rows, flip)
            projected = projected + jnp.dot(part, weight, preferred_element_type=jnp.float32)
        normed = layer_norm(projected, norm_gain[0])

        parity = tp % 2
        blocks = n_sp // 2
        width = normed.shape[1]
        column = width // n_sp
        halves = normed.astype(jnp.bfloat16).reshape(rows, blocks, 2, column)
        mine_half = lax.dynamic_index_in_dim(halves, parity, 2, keepdims=False)
        other_half = lax.dynamic_index_in_dim(halves, 1 - parity, 2, keepdims=False)
        own_rows = jnp.concatenate(
            [mine_half.reshape(rows, width // 2), other_half.reshape(rows, width // 2)], axis=1
        )

        def member(code):
            return lambda s, t: (s ^ (code % 2), t ^ (2 * (code // 2)))

        entered = jnp.concatenate([own_rows] + [send(own_rows, member(r)) for r in range(1, n_tp)])
        expanded = jnp.dot(
            entered[:, : width // 2], up_own, preferred_element_type=jnp.float32
        ) + jnp.dot(entered[:, width // 2 :], up_other, preferred_element_type=jnp.float32)
        hidden = jnp.square(jnp.maximum(expanded, 0.0)).astype(jnp.bfloat16)
        sums = []
        for weight in (down_own, down_other):
            for block in range(blocks):
                share = jnp.dot(hidden, weight[block], preferred_element_type=jnp.float32)
                half_share = share.astype(jnp.bfloat16)
                summed = share[:rows]
                for r in range(1, n_tp):
                    moved = send(half_share[r * rows : (r + 1) * rows], member(r))
                    summed = summed + moved.astype(jnp.float32)
                sums.append(summed)
        own_sum = jnp.stack(sums[:blocks], axis=1)
        other_sum = jnp.stack(sums[blocks:], axis=1)
        even = parity == 0
        mixed_sum = jnp.stack(
            [jnp.where(even, own_sum, other_sum), jnp.where(even, other_sum, own_sum)], axis=2
        ).reshape(rows, width)
        return layer_norm(normed + mixed_sum, norm_gain[1]).astype(jnp.bfloat16)

    return jax.shard_map(
        local,
        mesh=mesh,
        in_specs=(
            P("sp", "tp", None),
            P("sp", "tp", None),
            P("sp", "tp", None),
            P("sp", "tp", None),
            P("sp", "tp", None),
            P("sp", "tp", None),
            P(None, "tp"),
            P(None, "tp", None),
            P(None, "tp", None, None),
            P(("sp", "tp"), None),
            P(),
            P("sp", "tp"),
            P("tp", "sp"),
        ),
        out_specs=P(("sp", "tp"), None),
        check_vma=False,
    )
```

```python
import functools
import math

import jax
import jax.numpy as jnp
from jax import lax
from jax.experimental import pallas as pl
from jax.experimental.pallas import tpu as pltpu
from jax.sharding import PartitionSpec as P

EPSILON = 1e-05
LOG2_E = math.log2(math.e)
AXES = ("sp", "tp")
QUERY_BLOCK = 256


def layer_norm(activations, scales):
    average = jnp.mean(activations, axis=-1, keepdims=True)
    centred = activations - average
    spread = jnp.mean(centred * centred, axis=-1, keepdims=True)
    return centred * lax.rsqrt(spread + EPSILON) * scales


def attend_body(*refs, pieces, first, last):
    scal_ref, mask_ref, gain_ref, low_ref, high_ref = refs[:5]
    piece_refs = refs[5 : 5 + 2 * pieces]
    state_ref = None if first else refs[5 + 2 * pieces]
    out_ref = refs[-1]
    rows = low_ref.shape[0]
    value_size = gain_ref.shape[1]
    queries = jnp.concatenate([low_ref[...], high_ref[...]], axis=1)
    maps = [queries * mask_ref[c : c + 1, :] for c in range(2)]
    scale = scal_ref[0]
    upper = lax.broadcasted_iota(jnp.int32, (rows, 128), 1) >= 64
    running = [None, None]
    if not first:
        for c in range(2):
            kept = state_ref[c * rows : (c + 1) * rows, value_size:]
            top = jnp.max(jnp.where(upper, -jnp.inf, kept), axis=-1, keepdims=True)
            total = jnp.max(jnp.where(upper, kept, -jnp.inf), axis=-1, keepdims=True)
            running[c] = (state_ref[c * rows : (c + 1) * rows, :value_size], total, top)

    def score(piece, c):
        packed, key_high = piece_refs[2 * piece : 2 * piece + 2]
        keys = jnp.concatenate([packed[:, : key_high.shape[1]], key_high[...]], axis=1)
        return lax.dot_general(
            maps[c], keys, (((1,), (1,)), ((), ())), preferred_element_type=jnp.float32
        )

    def absorb(piece, c, scores):
        packed, key_high = piece_refs[2 * piece : 2 * piece + 2]
        values = packed[:, key_high.shape[1] :]
        scores = scores * scale
        newest = jnp.max(scores, axis=-1, keepdims=True)
        if running[c] is not None:
            newest = jnp.maximum(running[c][2], newest)
        weights = jnp.exp2(scores - newest).astype(jnp.bfloat16)
        extended = jnp.concatenate([values, jnp.ones_like(values)], axis=1)
        summed = jnp.dot(weights, extended, preferred_element_type=jnp.float32)
        numerator, total = summed[:, :value_size], summed[:, value_size:]
        if running[c] is not None:
            factor = jnp.exp2(running[c][2] - newest)
            numerator = running[c][0] * factor + numerator
            total = running[c][1] * factor + total
        running[c] = (numerator, total, newest)

    items = [(piece, c) for piece in range(pieces) for c in range(2)]
    waiting = score(*items[0])
    for item, following in zip(items, items[1:] + [None]):
        ahead = score(*following) if following else None
        absorb(*item, waiting)
        waiting = ahead
    if last:
        ratio = [numerator / total for numerator, total, _ in running]
        attended = ratio[0] - scal_ref[1] * ratio[1]
        mean_square = jnp.mean(attended * attended, axis=-1, keepdims=True)
        scaled = attended * lax.rsqrt(mean_square + EPSILON) * gain_ref[...]
        out_ref[...] = scaled.astype(out_ref.dtype)
    else:
        for c, (numerator, total, top) in enumerate(running):
            out_ref[c * rows : (c + 1) * rows, :value_size] = numerator
            out_ref[c * rows : (c + 1) * rows, value_size:] = jnp.where(upper, total, top)


def attend(scalars, masks, gain, query_low, query_high, pieces, state, last):
    count, wide = query_low.shape
    value_size = gain.shape[1]
    flat = [array for piece in pieces for array in piece]
    length = sum(piece[1].shape[0] for piece in pieces)
    state_width = value_size + 128
    state_spec = pl.BlockSpec((2 * QUERY_BLOCK, state_width), lambda i: (i, 0))
    operands = [scalars, masks, gain, query_low, query_high, *flat]
    in_specs = [
        pl.BlockSpec(memory_space=pltpu.SMEM),
        pl.BlockSpec((2, 2 * wide), lambda i: (0, 0)),
        pl.BlockSpec((1, value_size), lambda i: (0, 0)),
        pl.BlockSpec((QUERY_BLOCK, wide), lambda i: (i, 0)),
        pl.BlockSpec((QUERY_BLOCK, wide), lambda i: (i, 0)),
        *(pl.BlockSpec(array.shape, lambda i: (0, 0)) for array in flat),
    ]
    if state is not None:
        operands.append(state)
        in_specs.append(state_spec)
    if last:
        out_spec = pl.BlockSpec((QUERY_BLOCK, value_size), lambda i: (i, 0))
        out_shape = jax.ShapeDtypeStruct((count, value_size), jnp.bfloat16)
    else:
        out_spec = state_spec
        out_shape = jax.ShapeDtypeStruct((2 * count, state_width), jnp.float32)
    return pl.pallas_call(
        functools.partial(attend_body, pieces=len(pieces), first=state is None, last=last),
        grid=(count // QUERY_BLOCK,),
        in_specs=in_specs,
        out_specs=out_spec,
        out_shape=out_shape,
        compiler_params=pltpu.CompilerParams(vmem_limit_bytes=40 * 1024 * 1024),
        cost_estimate=pl.CostEstimate(
            flops=8 * count * length * (2 * wide + value_size),
            bytes_accessed=2 * (count + length) * 3 * wide + 16 * count * state_width,
            transcendentals=2 * count * length,
        ),
        name="attend",
    )(*operands)


def project_body(order_ref, *refs, members, blocks):
    parts, weights = refs[:members], refs[members : 2 * members]
    residual_ref, gain_ref, normed_ref, half_ref, scratch_ref = refs[2 * members :]
    projected = residual_ref[...].astype(jnp.float32)
    for part, weight in zip(parts, weights):
        projected = projected + jnp.dot(part[...], weight[...], preferred_element_type=jnp.float32)
    normed = layer_norm(projected, gain_ref[...])
    column = normed.shape[1] // blocks
    for block in range(blocks):
        scratch_ref[block] = normed[:, block * column : (block + 1) * column]
    for block in range(blocks):
        moved = scratch_ref[order_ref[block]]
        normed_ref[:, block * column : (block + 1) * column] = moved
        half_ref[:, block * column : (block + 1) * column] = moved.astype(half_ref.dtype)


def project(order, parts, weights, residual, gain):
    rows, width = residual.shape
    blocks = order.shape[0]
    vmem = pl.BlockSpec(memory_space=pltpu.VMEM)
    return pl.pallas_call(
        functools.partial(project_body, members=len(parts), blocks=blocks),
        in_specs=[pl.BlockSpec(memory_space=pltpu.SMEM)] + [vmem] * (2 * len(parts) + 2),
        out_specs=(vmem, vmem),
        out_shape=(
            jax.ShapeDtypeStruct((rows, width), jnp.float32),
            jax.ShapeDtypeStruct((rows, width), jnp.bfloat16),
        ),
        scratch_shapes=[pltpu.VMEM((blocks, rows, width // blocks), jnp.float32)],
        compiler_params=pltpu.CompilerParams(vmem_limit_bytes=40 * 1024 * 1024),
        cost_estimate=pl.CostEstimate(
            flops=2 * rows * width * sum(w.shape[0] for w in weights),
            bytes_accessed=2 * width * sum(w.shape[0] for w in weights),
            transcendentals=0,
        ),
        name="project",
    )(order, *parts, *weights, residual, gain)


def expand_body(*refs, members):
    entered = jnp.concatenate([ref[...] for ref in refs[:members]], axis=0)
    weights = refs[members:-1]
    size = weights[0].shape[0]
    total = None
    for index, ref in enumerate(weights):
        part = jnp.dot(
            entered[:, index * size : (index + 1) * size],
            ref[...],
            preferred_element_type=jnp.float32,
        )
        total = part if total is None else total + part
    refs[-1][...] = jnp.square(jnp.maximum(total, 0.0)).astype(refs[-1].dtype)


def expand(members, weights, tile):
    rows, width = members[0].shape
    size, hidden = weights[0].shape
    count = rows * len(members)
    return pl.pallas_call(
        functools.partial(expand_body, members=len(members)),
        grid=(hidden // tile,),
        in_specs=[pl.BlockSpec((rows, width), lambda j: (0, 0)) for _ in members]
        + [pl.BlockSpec((size, tile), lambda j: (0, j)) for _ in weights],
        out_specs=pl.BlockSpec((count, tile), lambda j: (0, j)),
        out_shape=jax.ShapeDtypeStruct((count, hidden), jnp.bfloat16),
        compiler_params=pltpu.CompilerParams(vmem_limit_bytes=40 * 1024 * 1024),
        cost_estimate=pl.CostEstimate(
            flops=2 * count * width * hidden,
            bytes_accessed=2 * (count * width + width * hidden + count * hidden),
            transcendentals=0,
        ),
        name="expand",
    )(*members, *weights)


def contract_body(hidden_ref, *refs):
    out_ref = refs[-1]
    column = refs[0].shape[1]
    for index, ref in enumerate(refs[:-1]):
        part = jnp.dot(hidden_ref[...], ref[...], preferred_element_type=jnp.float32)
        out_ref[:, index * column : (index + 1) * column] = part.astype(out_ref.dtype)


def contract(hidden, weights, row_block):
    count, size = hidden.shape
    column = weights[0].shape[1]
    width = column * len(weights)
    return pl.pallas_call(
        contract_body,
        grid=(count // row_block,),
        in_specs=[pl.BlockSpec((row_block, size), lambda i: (i, 0))]
        + [pl.BlockSpec((size, column), lambda i: (0, 0)) for _ in weights],
        out_specs=pl.BlockSpec((row_block, width), lambda i: (i, 0)),
        out_shape=jax.ShapeDtypeStruct((count, width), jnp.bfloat16),
        compiler_params=pltpu.CompilerParams(vmem_limit_bytes=40 * 1024 * 1024),
        cost_estimate=pl.CostEstimate(
            flops=2 * count * size * width,
            bytes_accessed=2 * (count * size + size * width + count * width),
            transcendentals=0,
        ),
        name="contract",
    )(hidden, *weights)


def solution(mesh):
    n_sp, n_tp = mesh.shape["sp"], mesh.shape["tp"]

    def pairs(move):
        listed = []
        for s in range(n_sp):
            for t in range(n_tp):
                target = move(s, t)
                if target is not None:
                    listed.append((s * n_tp + t, target[0] * n_tp + target[1]))
        return listed

    def send(array, move):
        return lax.ppermute(array, AXES, pairs(move))

    def local(
        query_first,
        key_first,
        value_first,
        query_second,
        key_second,
        value_second,
        mix_lambda,
        head_gain,
        out_weight,
        residual,
        norm_gain,
        up_weight,
        down_weight,
    ):
        tok, heads, wide = query_first.shape
        size_first, size_second = wide // 2, query_second.shape[2] // 2
        value_size = value_first.shape[2]
        ways = 2 * heads
        stride = n_sp // ways
        sp, tp = lax.axis_index("sp"), lax.axis_index("tp")
        mine = sp // stride
        is_second = mine >= heads
        place, parity = sp // 2, tp % 2
        line = n_sp // 2

        def swap(s, t):
            return (s - s % 2 + t % 2, t - t % 2 + s % 2) if s % 2 != t % 2 else None

        def swapped(block):
            moved = send(block, swap)
            return jnp.where(sp % 2 == tp % 2, block, moved)

        def core(s, t):
            return (s, t ^ 1)

        def along(step, hops):
            def move(s, t):
                z = s // 2
                came = z if step > 0 else line - 1 - z
                inside = 0 <= z + step < line
                return (s + 2 * step, t) if inside and came >= hops else None

            return move

        def shifted(step):
            return lambda s, t: ((s + step * stride) % n_sp, t)

        def only_high(move):
            def moved(s, t):
                target = move(s, t)
                return target if target[0] // stride >= heads else None

            return moved

        def across(step):
            return lambda s, t: (s - s % stride + (s % stride + step) % stride, t)

        def pick(array, way):
            return lax.dynamic_index_in_dim(array, way, 0, keepdims=False)

        def by_head(array):
            return jnp.transpose(array, (1, 0, 2))

        up_block = swapped(up_weight)
        down_block = swapped(down_weight)

        query_both, key_both = by_head(query_second), by_head(key_second)
        query_main = jnp.concatenate([by_head(query_first), query_both[:, :, :wide]])
        key_main = jnp.concatenate([by_head(key_first), key_both[:, :, :wide]])
        value_main = jnp.concatenate([by_head(value_first), by_head(value_second)])
        query_high, key_high = query_both[:, :, wide:], key_both[:, :, wide:]

        ways_of = [(mine + step) % ways for step in range(ways)]
        uppers = [jnp.maximum(way - heads, 0) for way in ways_of]

        def own_high(array):
            part = pick(array, uppers[0])
            return jnp.where(is_second, part, jnp.zeros_like(part))

        lows, highs = [pick(query_main, mine)], [own_high(query_high)]
        for step in range(1, ways):
            lows.append(send(pick(query_main, ways_of[step]), shifted(step)))
            part = pick(query_high, uppers[step])
            highs.append(send(part, only_high(shifted(step))))
        pieces = []
        packed_rows = []
        for step in range(ways):
            packed = jnp.concatenate(
                [pick(key_main, ways_of[step]), pick(value_main, ways_of[step])], axis=1
            )
            if step == 0:
                upper = own_high(key_high)
            else:
                packed = send(packed, shifted(step))
                upper = send(pick(key_high, uppers[step]), only_high(shifted(step)))
            packed_rows.append((packed, upper))
        for packed, upper in packed_rows:
            group = [(packed, upper)]
            for other in range(1, stride):
                moved = send(packed, across(other))
                moved_high = send(upper, only_high(across(other)))
                group.append((moved, moved_high))
            pieces.append(group)

        chains = {"up": (up_block, [], []), "down": (down_block, [], [])}
        for hop in range(line - 1):
            for (block, rising, falling) in chains.values():
                ahead = rising[-1] if hop else block
                behind = falling[-1] if hop else block
                rising.append(send(ahead, along(1, hop)))
                falling.append(send(behind, along(-1, hop)))

        rises = place >= line // 2
        far = jnp.maximum(place, line - 1 - place)

        def arrived(kind):
            block, rising, falling = chains[kind]
            slots = [block]
            for k in range(line - 1):
                candidates = [(rising[k], falling[k])]
                candidates += [(falling[j], rising[j]) for j in range(k - line // 2 + 1)]
                if len(candidates) > 1:
                    candidates = lax.optimization_barrier(candidates)
                slot = jnp.where(rises, *candidates[0])
                for j, pair in enumerate(candidates[1:]):
                    slot = jnp.where(k - far == j, jnp.where(rises, *pair), slot)
                slots.append(slot)
            return [(part, send(part, core)) for part in slots]

        table = [[z] for z in range(line)]
        for z, row in enumerate(table):
            below, above = list(range(z - 1, -1, -1)), list(range(z + 1, line))
            row += below + above if z >= line // 2 else above + below
        inverse = [[row.index(z) for z in range(line)] for row in table]
        block_of = jnp.asarray(table, jnp.int32)[place]
        slot_of = jnp.asarray(inverse, jnp.int32)[place]

        lanes = jnp.arange(2 * wide)[None, :]
        half = jnp.where(is_second, wide, size_first)
        masks = jnp.concatenate([lanes < half, lanes >= half]).astype(jnp.bfloat16)
        scale = jnp.where(is_second, 1.0 / math.sqrt(size_second), 1.0 / math.sqrt(size_first))
        way_lambda = pick(mix_lambda.reshape(ways), mine)
        way_gain = pick(head_gain.reshape(ways, value_size), mine)[None, :]
        scalars = jnp.stack([scale * LOG2_E, way_lambda]).astype(jnp.float32)
        query_low, query_up = jnp.concatenate(lows), jnp.concatenate(highs)
        state = None
        for step in range(ways):
            state = attend(
                scalars, masks, way_gain, query_low, query_up, pieces[step], state, step == ways - 1
            )
        head_out = state

        rows = tok // n_tp
        weight_rows = out_weight.reshape(ways * value_size, out_weight.shape[-1])
        out_weights = [weight_rows]
        for bit in range(1, n_tp):
            flip = core if bit % 2 else lambda s, t, bit=bit: (s, t ^ bit)
            source = out_weights[bit - 1] if bit % 2 else weight_rows
            out_weights.append(send(source, flip))
        returned = []
        for step in range(ways):
            part = head_out[step * tok : (step + 1) * tok]
            returned.append(part if step == 0 else send(part, shifted(-step)))
        returned = jnp.stack(returned)
        ordered = jnp.concatenate([pick(returned, (w - mine) % ways) for w in range(ways)], axis=1)
        width = residual.shape[1]
        column = width // n_sp
        sides = (parity, 1 - parity)
        arrival = jnp.stack([2 * block_of[k] + y for k in range(line) for y in sides]).astype(jnp.int32)
        parts = []
        for bit in range(n_tp):
            part = lax.dynamic_slice_in_dim(ordered, (tp ^ bit) * rows, rows, 0)
            flip = lambda s, t, bit=bit: (s, t ^ bit)
            parts.append(send(part, flip) if bit else part)
        normed, own_rows = project(arrival, parts, out_weights, residual, norm_gain[0:1])
        gain_blocks = norm_gain[1].reshape(n_sp, column)
        last_gain = jnp.concatenate([pick(gain_blocks, arrival[k]) for k in range(n_sp)])[None, :]

        def member(code):
            return lambda s, t: (s ^ (code % 2), t ^ (2 * (code // 2)))

        members = [own_rows] + [send(own_rows, member(r)) for r in range(1, n_tp)]
        up_slots = [weight for pair in arrived("up") for weight in pair]
        hidden = expand(members, up_slots, 512)
        down_slots = arrived("down")
        sums = []
        for slots in (down_slots[:-1], down_slots[-1:]):
            share = contract(hidden, [weight for pair in slots for weight in pair], rows)
            summed = share[:rows].astype(jnp.float32)
            for r in range(1, n_tp):
                moved = send(share[r * rows : (r + 1) * rows], member(r))
                summed = summed + moved.astype(jnp.float32)
            sums.append(summed)
        mixed = layer_norm(normed + jnp.concatenate(sums, axis=1), last_gain).astype(jnp.bfloat16)
        mixed = mixed.reshape(rows, n_sp, column).swapaxes(0, 1)
        placed = [
            pick(mixed, 2 * slot_of[z] + (parity if y == 0 else 1 - parity))
            for z in range(line)
            for y in range(2)
        ]
        return jnp.concatenate(placed, axis=1)

    return jax.shard_map(
        local,
        mesh=mesh,
        in_specs=(
            P("sp", "tp", None),
            P("sp", "tp", None),
            P("sp", "tp", None),
            P("sp", "tp", None),
            P("sp", "tp", None),
            P("sp", "tp", None),
            P(None, "tp"),
            P(None, "tp", None),
            P(None, "tp", None, None),
            P(("sp", "tp"), None),
            P(),
            P("sp", "tp"),
            P("tp", "sp"),
        ),
        out_specs=P(("sp", "tp"), None),
        check_vma=False,
    )
```

```python
import functools
import math

import jax
import jax.numpy as jnp
from jax import lax
from jax.experimental import pallas as pl
from jax.experimental.pallas import tpu as pltpu
from jax.sharding import PartitionSpec as P

EPSILON = 1e-05
LOG2_E = math.log2(math.e)
AXES = ("sp", "tp")
QUERY_BLOCK = 256


def layer_norm(activations, scales):
    average = jnp.mean(activations, axis=-1, keepdims=True)
    centred = activations - average
    spread = jnp.mean(centred * centred, axis=-1, keepdims=True)
    return centred * lax.rsqrt(spread + EPSILON) * scales


def attend_body(*refs, pieces, first, last):
    scal_ref, mask_ref, gain_ref, low_ref, high_ref = refs[:5]
    piece_refs = refs[5 : 5 + 2 * pieces]
    state_ref = None if first else refs[5 + 2 * pieces]
    out_ref = refs[-1]
    rows = low_ref.shape[0]
    value_size = gain_ref.shape[1]
    queries = jnp.concatenate([low_ref[...], high_ref[...]], axis=1)
    maps = [queries * mask_ref[c : c + 1, :] for c in range(2)]
    scale = scal_ref[0]
    upper = lax.broadcasted_iota(jnp.int32, (rows, 128), 1) >= 64
    running = [None, None]
    if not first:
        for c in range(2):
            kept = state_ref[c * rows : (c + 1) * rows, value_size:]
            top = jnp.max(jnp.where(upper, -jnp.inf, kept), axis=-1, keepdims=True)
            total = jnp.max(jnp.where(upper, kept, -jnp.inf), axis=-1, keepdims=True)
            running[c] = (state_ref[c * rows : (c + 1) * rows, :value_size], total, top)

    def score(piece, c):
        packed, key_high = piece_refs[2 * piece : 2 * piece + 2]
        keys = jnp.concatenate([packed[:, : key_high.shape[1]], key_high[...]], axis=1)
        return lax.dot_general(
            maps[c], keys, (((1,), (1,)), ((), ())), preferred_element_type=jnp.float32
        )

    def absorb(piece, c, scores):
        packed, key_high = piece_refs[2 * piece : 2 * piece + 2]
        values = packed[:, key_high.shape[1] :]
        scores = scores * scale
        newest = jnp.max(scores, axis=-1, keepdims=True)
        if running[c] is not None:
            newest = jnp.maximum(running[c][2], newest)
        weights = jnp.exp2(scores - newest).astype(jnp.bfloat16)
        extended = jnp.concatenate([values, jnp.ones_like(values)], axis=1)
        summed = jnp.dot(weights, extended, preferred_element_type=jnp.float32)
        numerator, total = summed[:, :value_size], summed[:, value_size:]
        if running[c] is not None:
            factor = jnp.exp2(running[c][2] - newest)
            numerator = running[c][0] * factor + numerator
            total = running[c][1] * factor + total
        running[c] = (numerator, total, newest)

    items = [(piece, c) for piece in range(pieces) for c in range(2)]
    waiting = score(*items[0])
    for item, following in zip(items, items[1:] + [None]):
        ahead = score(*following) if following else None
        absorb(*item, waiting)
        waiting = ahead
    if last:
        ratio = [numerator / total for numerator, total, _ in running]
        attended = ratio[0] - scal_ref[1] * ratio[1]
        mean_square = jnp.mean(attended * attended, axis=-1, keepdims=True)
        scaled = attended * lax.rsqrt(mean_square + EPSILON) * gain_ref[...]
        out_ref[...] = scaled.astype(out_ref.dtype)
    else:
        for c, (numerator, total, top) in enumerate(running):
            out_ref[c * rows : (c + 1) * rows, :value_size] = numerator
            out_ref[c * rows : (c + 1) * rows, value_size:] = jnp.where(upper, total, top)


def attend(scalars, masks, gain, query_low, query_high, pieces, state, last):
    count, wide = query_low.shape
    value_size = gain.shape[1]
    flat = [array for piece in pieces for array in piece]
    length = sum(piece[1].shape[0] for piece in pieces)
    state_width = value_size + 128
    state_spec = pl.BlockSpec((2 * QUERY_BLOCK, state_width), lambda i: (i, 0))
    operands = [scalars, masks, gain, query_low, query_high, *flat]
    in_specs = [
        pl.BlockSpec(memory_space=pltpu.SMEM),
        pl.BlockSpec((2, 2 * wide), lambda i: (0, 0)),
        pl.BlockSpec((1, value_size), lambda i: (0, 0)),
        pl.BlockSpec((QUERY_BLOCK, wide), lambda i: (i, 0)),
        pl.BlockSpec((QUERY_BLOCK, wide), lambda i: (i, 0)),
        *(pl.BlockSpec(array.shape, lambda i: (0, 0)) for array in flat),
    ]
    if state is not None:
        operands.append(state)
        in_specs.append(state_spec)
    if last:
        out_spec = pl.BlockSpec((QUERY_BLOCK, value_size), lambda i: (i, 0))
        out_shape = jax.ShapeDtypeStruct((count, value_size), jnp.bfloat16)
    else:
        out_spec = state_spec
        out_shape = jax.ShapeDtypeStruct((2 * count, state_width), jnp.float32)
    return pl.pallas_call(
        functools.partial(attend_body, pieces=len(pieces), first=state is None, last=last),
        grid=(count // QUERY_BLOCK,),
        in_specs=in_specs,
        out_specs=out_spec,
        out_shape=out_shape,
        compiler_params=pltpu.CompilerParams(vmem_limit_bytes=40 * 1024 * 1024),
        cost_estimate=pl.CostEstimate(
            flops=8 * count * length * (2 * wide + value_size),
            bytes_accessed=2 * (count + length) * 3 * wide + 16 * count * state_width,
            transcendentals=2 * count * length,
        ),
        name="attend",
    )(*operands)


def project_body(*refs, members):
    parts, weights = refs[:members], refs[members : 2 * members]
    residual_ref, gain_ref, normed_ref, half_ref = refs[2 * members :]
    projected = residual_ref[...].astype(jnp.float32)
    for part, weight in zip(parts, weights):
        projected = projected + jnp.dot(part[...], weight[...], preferred_element_type=jnp.float32)
    normed = layer_norm(projected, gain_ref[...])
    normed_ref[...] = normed
    half_ref[...] = normed.astype(half_ref.dtype)


def project(parts, weights, residual, gain):
    rows, width = residual.shape
    vmem = pl.BlockSpec(memory_space=pltpu.VMEM)
    return pl.pallas_call(
        functools.partial(project_body, members=len(parts)),
        in_specs=[vmem] * (2 * len(parts) + 2),
        out_specs=(vmem, vmem),
        out_shape=(
            jax.ShapeDtypeStruct((rows, width), jnp.float32),
            jax.ShapeDtypeStruct((rows, width), jnp.bfloat16),
        ),
        compiler_params=pltpu.CompilerParams(vmem_limit_bytes=40 * 1024 * 1024),
        cost_estimate=pl.CostEstimate(
            flops=2 * rows * width * sum(w.shape[0] for w in weights),
            bytes_accessed=2 * width * sum(w.shape[0] for w in weights),
            transcendentals=0,
        ),
        name="project",
    )(*parts, *weights, residual, gain)


def feed_body(order_ref, *refs, members, pieces):
    rows_refs, weights = refs[:members], refs[members : members + pieces]
    out_ref, entered_ref, total_ref = refs[-3:]
    step = pl.program_id(0)
    size, tile = weights[0].shape[0] // 2, weights[0].shape[1]

    @pl.when(step == 0)
    def _():
        entered = jnp.concatenate([ref[...] for ref in rows_refs], axis=0)
        for block in range(pieces):
            entered_ref[block] = entered[:, block * size : (block + 1) * size]
        total_ref[...] = jnp.zeros_like(total_ref)

    expanded = None
    for i in range(0, pieces, 2):
        left = jnp.concatenate([entered_ref[order_ref[i]], entered_ref[order_ref[i + 1]]], axis=1)
        right = jnp.concatenate([weights[i][:size], weights[i + 1][:size]], axis=0)
        part = jnp.dot(left, right, preferred_element_type=jnp.float32)
        expanded = part if expanded is None else expanded + part
    hidden = jnp.square(jnp.maximum(expanded, 0.0)).astype(jnp.bfloat16)
    for i in range(0, pieces, 2):
        right = jnp.concatenate(
            [
                jnp.concatenate([weights[j][size:, a : a + size] for a in range(0, tile, size)], axis=0)
                for j in (i, i + 1)
            ],
            axis=1,
        )
        part = jnp.dot(hidden, right, preferred_element_type=jnp.float32)
        total_ref[order_ref[i]] += part[:, :size]
        total_ref[order_ref[i + 1]] += part[:, size:]

    @pl.when(step == pl.num_programs(0) - 1)
    def _():
        for block in range(pieces):
            out_ref[:, block * size : (block + 1) * size] = total_ref[block].astype(out_ref.dtype)


def feed(order, members, weights, tile):
    rows, width = members[0].shape
    size, hidden = weights[0].shape[0] // 2, weights[0].shape[1]
    count = rows * len(members)
    pieces = len(weights)
    return pl.pallas_call(
        functools.partial(feed_body, members=len(members), pieces=pieces),
        grid=(hidden // tile,),
        in_specs=[pl.BlockSpec(memory_space=pltpu.SMEM)]
        + [pl.BlockSpec((rows, width), lambda j: (0, 0)) for _ in members]
        + [pl.BlockSpec((2 * size, tile), lambda j: (0, j)) for _ in weights],
        out_specs=pl.BlockSpec((count, width), lambda j: (0, 0)),
        out_shape=jax.ShapeDtypeStruct((count, width), jnp.bfloat16),
        scratch_shapes=[
            pltpu.VMEM((pieces, count, size), jnp.bfloat16),
            pltpu.VMEM((pieces, count, size), jnp.float32),
        ],
        compiler_params=pltpu.CompilerParams(vmem_limit_bytes=40 * 1024 * 1024),
        cost_estimate=pl.CostEstimate(
            flops=4 * count * width * hidden,
            bytes_accessed=4 * (count * width + width * hidden),
            transcendentals=0,
        ),
        name="feed",
    )(order, *members, *weights)


def member_groups(n_tp):
    return ([0], list(range(1, n_tp - 1)), [n_tp - 1])


def solution(mesh):
    n_sp, n_tp = mesh.shape["sp"], mesh.shape["tp"]

    def pairs(move):
        listed = []
        for s in range(n_sp):
            for t in range(n_tp):
                target = move(s, t)
                if target is not None:
                    listed.append((s * n_tp + t, target[0] * n_tp + target[1]))
        return listed

    def send(array, move):
        return lax.ppermute(array, AXES, pairs(move))

    def local(
        query_first,
        key_first,
        value_first,
        query_second,
        key_second,
        value_second,
        mix_lambda,
        head_gain,
        out_weight,
        residual,
        norm_gain,
        up_weight,
        down_weight,
    ):
        tok, heads, wide = query_first.shape
        size_first, size_second = wide // 2, query_second.shape[2] // 2
        value_size = value_first.shape[2]
        ways = 2 * heads
        stride = n_sp // ways
        sp, tp = lax.axis_index("sp"), lax.axis_index("tp")
        mine = sp // stride
        is_second = mine >= heads
        place, parity = sp // 2, tp % 2
        line = n_sp // 2

        def core(s, t):
            return (s, t ^ 1)

        def along(step):
            return lambda s, t: ((s + 2 * step) % n_sp, t)

        def beside(s, t):
            return (s ^ 1, t)

        def shifted(step):
            return lambda s, t: ((s + step * stride) % n_sp, t)

        def only_high(move):
            def moved(s, t):
                target = move(s, t)
                return target if target[0] // stride >= heads else None

            return moved

        def across(step):
            return lambda s, t: (s - s % stride + (s % stride + step) % stride, t)

        def pick(array, way):
            return lax.dynamic_index_in_dim(array, way, 0, keepdims=False)

        def by_head(array):
            return jnp.transpose(array, (1, 0, 2))

        query_both, key_both = by_head(query_second), by_head(key_second)
        query_main = jnp.concatenate([by_head(query_first), query_both[:, :, :wide]])
        key_main = jnp.concatenate([by_head(key_first), key_both[:, :, :wide]])
        value_main = jnp.concatenate([by_head(value_first), by_head(value_second)])
        query_high, key_high = query_both[:, :, wide:], key_both[:, :, wide:]

        ways_of = [(mine + step) % ways for step in range(ways)]
        uppers = [jnp.maximum(way - heads, 0) for way in ways_of]

        def own_high(array):
            part = pick(array, uppers[0])
            return jnp.where(is_second, part, jnp.zeros_like(part))

        lows, highs = [pick(query_main, mine)], [own_high(query_high)]
        for step in range(1, ways):
            lows.append(send(pick(query_main, ways_of[step]), shifted(step)))
            part = pick(query_high, uppers[step])
            highs.append(send(part, only_high(shifted(step))))
        pieces = []
        packed_rows = []
        for step in range(ways):
            packed = jnp.concatenate(
                [pick(key_main, ways_of[step]), pick(value_main, ways_of[step])], axis=1
            )
            if step == 0:
                upper = own_high(key_high)
            else:
                packed = send(packed, shifted(step))
                upper = send(pick(key_high, uppers[step]), only_high(shifted(step)))
            packed_rows.append((packed, upper))
        for packed, upper in packed_rows:
            group = [(packed, upper)]
            for other in range(1, stride):
                moved = send(packed, across(other))
                moved_high = send(upper, only_high(across(other)))
                group.append((moved, moved_high))
            pieces.append(group)

        size = up_weight.shape[0] // 2

        def packed_half(half):
            up = lax.dynamic_slice_in_dim(up_weight, half * size, size, 0)
            down = lax.dynamic_slice_in_dim(down_weight, half * size, size, 1)
            squares = [down[a : a + size] for a in range(0, down.shape[0], size)]
            return jnp.concatenate([up, jnp.concatenate(squares, axis=1)], axis=0)

        own_half, other_half = packed_half(parity), send(packed_half(1 - parity), core)
        same = place % 2 == parity
        even, odd = jnp.where(same, own_half, other_half), jnp.where(same, other_half, own_half)
        weight_pieces = []
        for step in range(line):
            piece = even
            if step:
                piece = send(odd if step % 2 else even, along(step))
            for part in (piece, send(piece, beside)):
                weight_pieces += [part, send(part, core)]
        piece_order = jnp.stack(
            [
                2 * (2 * lax.rem(place - step + line, line) + (y + sp) % 2) + (c + tp) % 2
                for step in range(line)
                for y in range(2)
                for c in range(2)
            ]
        ).astype(jnp.int32)

        lanes = jnp.arange(2 * wide)[None, :]
        half = jnp.where(is_second, wide, size_first)
        masks = jnp.concatenate([lanes < half, lanes >= half]).astype(jnp.bfloat16)
        scale = jnp.where(is_second, 1.0 / math.sqrt(size_second), 1.0 / math.sqrt(size_first))
        way_lambda = pick(mix_lambda.reshape(ways), mine)
        way_gain = pick(head_gain.reshape(ways, value_size), mine)[None, :]
        scalars = jnp.stack([scale * LOG2_E, way_lambda]).astype(jnp.float32)
        query_low, query_up = jnp.concatenate(lows), jnp.concatenate(highs)
        state = None
        for step in range(ways):
            state = attend(
                scalars, masks, way_gain, query_low, query_up, pieces[step], state, step == ways - 1
            )
        head_out = state

        rows = tok // n_tp
        weight_rows = out_weight.reshape(ways * value_size, out_weight.shape[-1])
        out_weights = [weight_rows]
        for bit in range(1, n_tp):
            flip = core if bit % 2 else lambda s, t, bit=bit: (s, t ^ bit)
            source = out_weights[bit - 1] if bit % 2 else weight_rows
            out_weights.append(send(source, flip))
        returned = []
        for step in range(ways):
            part = head_out[step * tok : (step + 1) * tok]
            returned.append(part if step == 0 else send(part, shifted(-step)))
        returned = jnp.stack(returned)
        ordered = jnp.concatenate([pick(returned, (w - mine) % ways) for w in range(ways)], axis=1)
        parts = []
        for bit in range(n_tp):
            part = lax.dynamic_slice_in_dim(ordered, (tp ^ bit) * rows, rows, 0)
            flip = lambda s, t, bit=bit: (s, t ^ bit)
            parts.append(send(part, flip) if bit else part)
        normed, own_rows = project(parts, out_weights, residual, norm_gain[0:1])

        def member(code):
            return lambda s, t: (s ^ (2 * (code % 2)), t ^ (2 * (code // 2)))

        members = [own_rows] + [send(own_rows, member(r)) for r in range(1, n_tp)]
        mixed_sum = None
        for group in member_groups(n_tp):
            shares = feed(piece_order, [members[r] for r in group], weight_pieces, 512)
            for index, r in enumerate(group):
                share = shares[index * rows : (index + 1) * rows]
                if r:
                    share = send(share, member(r))
                share = share.astype(jnp.float32)
                mixed_sum = share if mixed_sum is None else mixed_sum + share
        return layer_norm(normed + mixed_sum, norm_gain[1]).astype(jnp.bfloat16)

    return jax.shard_map(
        local,
        mesh=mesh,
        in_specs=(
            P("sp", "tp", None),
            P("sp", "tp", None),
            P("sp", "tp", None),
            P("sp", "tp", None),
            P("sp", "tp", None),
            P("sp", "tp", None),
            P(None, "tp"),
            P(None, "tp", None),
            P(None, "tp", None, None),
            P(("sp", "tp"), None),
            P(),
            P("sp", "tp"),
            P("tp", "sp"),
        ),
        out_specs=P(("sp", "tp"), None),
        check_vma=False,
    )
```
